32 devices in a mesh: sp: 4 (over z), fs: 4 (over y, x), tp: 2 (over core).
Axes of the slice: x: 2, y: 2, z: 4, core: 2. Of those that a mesh axis runs over, the one named last changes fastest.
Arguments:
- tokens: bfloat16 [4, 1536, 2048], P('fs', ('sp', 'tp')), may hold values from -6 to 6
- norm_gain: float32 [2048], replicated, may hold values from 0.1 to 1.9
- conv_gate_w: bfloat16 [2048, 1024], P('sp', 'tp'), may hold values from -0.125 to 0.125
- conv_in_w: bfloat16 [2048, 1024], P('sp', 'tp'), may hold values from -0.125 to 0.125
- query_w: bfloat16 [2048, 1024], P('sp', 'tp'), may hold values from -0.125 to 0.125
- forget_w: bfloat16 [2048, 1024], P('sp', 'tp'), may hold values from -0.125 to 0.125
- value_w: bfloat16 [2048, 1024], P('sp', 'tp'), may hold values from -0.125 to 0.125
- conv_taps: float32 [3, 1024], P(None, 'tp'), may hold values from -3.5 to 3.5
- floor_gate: float32 [1024], P('tp'), may hold values from 0.93 to 1
- leak: float32 [4, 1536, 8], P('fs', 'sp', 'tp'), may hold values from -1.4 to 0
- head_gain: float32 [128], replicated, may hold values from 0.1 to 1.9
- conv_out_w: bfloat16 [1024, 2048], P('tp', 'fs'), may hold values from -0.125 to 0.125
- chain_out_w: bfloat16 [1024, 2048], P('tp', 'fs'), may hold values from -0.125 to 0.125
Outputs:
- mixed: bfloat16 [4, 1536, 2048], P('fs', ('sp', 'tp'))
The draws below stay inside these ranges and needn't reach their ends.
All inputs are finite; a program needn't handle non-finite values.
Results may differ from the reference program's by a relative error of at most 0.013.
Values may be sent and summed in bfloat16 or wider, within the bound.
A program may use at most 128 MiB of HBM per device.

```python
import jax
import jax.numpy as jnp
from jax import lax

D = 2048
CW = 1024
HEADS = 8
HEAD_DIM = 128
TOK = 384
BLOCK = 64
HW = 1024
SEQS = 4
LEN = 1536


def draw_floor_gate(key, part):
    base = jax.random.fold_in(key, 101)
    pick_key, fast_key, slow_key = jax.random.split(base, 3)
    fast_share = 0.5
    fast = jax.random.bernoulli(pick_key, fast_share, (HEADS, 1))
    fast_gap = jnp.exp(jax.random.uniform(fast_key, (HEADS, HEAD_DIM), jnp.float32, jnp.log(0.02), jnp.log(0.07)))
    slow_gap = jnp.exp(jax.random.uniform(slow_key, (HEADS, HEAD_DIM), jnp.float32, jnp.log(0.2), jnp.log(0.8))) / LEN
    return (1.0 - jnp.where(fast, fast_gap, slow_gap)).reshape(HEADS * HEAD_DIM).astype(jnp.float32)


def draw_leak(key, part):
    base = jax.random.fold_in(key, 202)
    rate_key, spot_key, depth_key = jax.random.split(base, 3)
    blocks = LEN // TOK
    rates = jnp.exp(jax.random.uniform(rate_key, (SEQS, blocks, 1, HEADS), jnp.float32, jnp.log(0.1), jnp.log(1.0))) / LEN
    constant_fading = -jnp.broadcast_to(rates, (SEQS, blocks, TOK, HEADS)).reshape(SEQS, LEN, HEADS)
    chosen_indices = jax.random.randint(spot_key, (SEQS, 1, HEADS, 2), 0, LEN)
    memory_width = jnp.log(jax.random.uniform(depth_key, (SEQS, 1, HEADS, 2), jnp.float32, 0.5, 0.8))
    sequence_slots = jnp.arange(LEN)[None, :, None, None]
    spike_clusters = jnp.sum(jnp.where(sequence_slots == chosen_indices, memory_width, 0.0), axis=3)
    return (constant_fading + spike_clusters).astype(jnp.float32)


def shard_levels(rng, dims, pieces, least, top_value):
    loudness = 1.0
    for position, parts in pieces:
        steps = jax.random.uniform(jax.random.fold_in(jax.random.fold_in(rng, 6), position), (parts,), jnp.float32, least / len(pieces), top_value / len(pieces))
        loudness = loudness * jnp.repeat(jnp.exp(steps), dims[position] // parts).reshape((-1,) + (1,) * (len(dims) - 1 - position))
    return loudness


def normal_values(stream_key, dims, scale, reach, cuts=(), dtype=jnp.bfloat16):
    values = jax.random.normal(stream_key, dims, jnp.float32) * scale
    if len(cuts) > 0:
        values = shard_levels(stream_key, dims, cuts, -0.22, 0.18) * values
    return jnp.clip(values, min=-reach, max=reach).astype(dtype)


def setup_inputs(seed: int = 0) -> dict:
    key_list = jax.random.split(jax.random.key(seed), 14)
    tokens = normal_values(key_list[0], (SEQS, LEN, D), 1.0, 6.0, ((0, 4), (1, 8)))
    norm_gain = jnp.clip(1.0 + 0.18 * jax.random.normal(key_list[1], (D,), jnp.float32), 0.1, 1.9)
    conv_gate_w = normal_values(key_list[2], (D, CW), D ** -0.5, 0.125, ((0, 4), (1, 2)))
    conv_in_w = normal_values(key_list[3], (D, CW), D ** -0.5, 0.125, ((0, 4), (1, 2)))
    query_w = normal_values(key_list[4], (D, HW), D ** -0.5, 0.125, ((0, 4), (1, 2)))
    forget_w = normal_values(key_list[5], (D, HW), D ** -0.5, 0.125, ((0, 4), (1, 2)))
    value_w = normal_values(key_list[6], (D, HW), D ** -0.5, 0.125, ((0, 4), (1, 2)))
    conv_taps = normal_values(key_list[7], (3, CW), 3 ** -0.5, 3.5, ((1, 2),), jnp.float32)
    floor_gate = draw_floor_gate(jax.random.fold_in(key_list[13], 71), 0)
    leak = draw_leak(jax.random.fold_in(key_list[13], 71), 0)
    head_gain = jnp.clip(1.0 + 0.18 * jax.random.normal(key_list[10], (HEAD_DIM,), jnp.float32), 0.1, 1.9)
    conv_out_w = normal_values(key_list[11], (CW, D), (CW + HW) ** -0.5, 0.125, ((0, 2), (1, 4)))
    chain_out_w = normal_values(key_list[12], (HW, D), (CW + HW) ** -0.5, 0.125, ((0, 2), (1, 4)))
    return {"tokens": tokens, "norm_gain": norm_gain, "conv_gate_w": conv_gate_w, "conv_in_w": conv_in_w, "query_w": query_w, "forget_w": forget_w, "value_w": value_w, "conv_taps": conv_taps, "floor_gate": floor_gate, "leak": leak, "head_gain": head_gain, "conv_out_w": conv_out_w, "chain_out_w": chain_out_w}


HIGH_ACCURACY = lax.Precision.HIGHEST

def norm_rows(matrix, norm_gain):
    values = matrix.astype(jnp.float32)
    center = values - lax.optimization_barrier(jnp.mean(values, axis=-1, keepdims=True))
    spread = lax.optimization_barrier(jnp.mean(center * center, axis=-1, keepdims=True))
    return (center * lax.rsqrt(spread + 1e-05) * norm_gain).astype(jnp.bfloat16)

def block_chain(query, keys, values, decay):
    heads, length, width = query.shape
    count = length // BLOCK

    def split_blocks(array):
        return array.reshape(heads, count, BLOCK, array.shape[-1]).transpose(1, 0, 2, 3)
    causal = jnp.tril(jnp.ones((BLOCK, BLOCK), jnp.float32))

    def advance(hidden_state, inputs):
        query_part, key_portion, value_portion, decay_part = inputs
        running_state = jnp.cumsum(decay_part, axis=1)
        scaled_query = query_part * jnp.exp(running_state)
        key_scaled = key_portion * jnp.exp(-running_state)
        scores = jnp.einsum('htk,hsk->hts', scaled_query, key_scaled, precision=HIGH_ACCURACY) * causal
        inside = jnp.einsum('hts,hsv->htv', scores, value_portion, precision=HIGH_ACCURACY)
        carried_state = jnp.einsum('rgn,rns->rgs', scaled_query, hidden_state, precision=HIGH_ACCURACY)
        final_state = running_state[:, -1:, :]
        state_update = jnp.einsum('qdm,qdt->qmt', key_portion * jnp.exp(final_state - running_state), value_portion, precision=HIGH_ACCURACY)
        return (jnp.exp(final_state[:, 0, :])[:, :, None] * hidden_state + state_update, inside + carried_state)
    initial = jnp.zeros((heads, width, values.shape[-1]), jnp.float32)
    hidden_state, layer_results = lax.scan(advance, initial, (split_blocks(query), split_blocks(keys), split_blocks(values), split_blocks(decay)))
    return (layer_results.transpose(1, 0, 2, 3).reshape(heads, length, values.shape[-1]), hidden_state)

def reference(tokens, norm_gain, conv_gate_w, conv_in_w, query_w, forget_w, value_w, conv_taps, floor_gate, leak, head_gain, conv_out_w, chain_out_w):
    seqs, length, width = tokens.shape
    normed = norm_rows(tokens.reshape(seqs * length, width), norm_gain)

    def project(weight):
        product = jnp.dot(normed, weight, preferred_element_type=jnp.float32)
        return product.astype(jnp.bfloat16).reshape(seqs, length, weight.shape[1])
    second_gate = project(conv_gate_w)
    signal = project(conv_in_w)
    query_raw = project(query_w)
    forget_raw = project(forget_w)
    value_raw = project(value_w)
    margin = conv_taps.shape[0] - 1
    padded = jnp.pad(signal.astype(jnp.float32), ((0, 0), (margin, 0), (0, 0)))
    filtered = jnp.zeros((seqs, length, signal.shape[2]), jnp.float32)
    for offset in range(margin + 1):
        filtered = filtered + conv_taps[offset] * padded[:, offset:offset + length]
    conv_mix = (second_gate.astype(jnp.float32) * filtered).astype(jnp.bfloat16)

    def chain_sequence(inputs):
        query_rows, forget_rows, value_rows, leak_rows = inputs

        def by_head(array):
            return array.astype(jnp.float32).reshape(length, HEADS, HEAD_DIM).transpose(1, 0, 2)
        floor = floor_gate.reshape(HEADS, 1, HEAD_DIM)
        logits = by_head(forget_rows)
        retain = floor + (1.0 - floor) * jax.nn.sigmoid(logits)
        keys = (1.0 - floor) * jax.nn.sigmoid(-logits)
        decay = jnp.log(retain) + leak_rows.T[:, :, None]
        layer_results, _ = block_chain(jax.nn.silu(by_head(query_rows)), keys, by_head(value_rows), decay)
        scale = lax.rsqrt(lax.optimization_barrier(jnp.mean(layer_results * layer_results, axis=-1, keepdims=True)) + 1e-06)
        normal_out = layer_results * scale * head_gain
        return normal_out.transpose(1, 0, 2).reshape(length, HEADS * HEAD_DIM).astype(jnp.bfloat16)
    chain_mix = lax.map(chain_sequence, (query_raw, forget_raw, value_raw, leak))
    mixed = jnp.dot(conv_mix.reshape(seqs * length, -1), conv_out_w, preferred_element_type=jnp.float32)
    mixed = mixed + jnp.dot(chain_mix.reshape(seqs * length, -1), chain_out_w, preferred_element_type=jnp.float32)
    return mixed.astype(jnp.bfloat16).reshape(seqs, length, width)
```

```python
import functools

import jax
import jax.numpy as jnp
from jax import lax
from jax.experimental import pallas as pl
from jax.experimental.pallas import tpu as pltpu
from jax.sharding import PartitionSpec as P

MESH = pl.DeviceIdType.MESH
BF = jnp.bfloat16
F32 = jnp.float32
NT = (((1,), (1,)), ((), ()))
TN = (((0,), (0,)), ((), ()))
GATE, SIGNAL, QUERY, FORGET, VALUE = 4, 3, 1, 0, 2


def kernel(
    ns, nf,
    tok, gain, w0, w1, w2, w3, w4, taps, floor, leak, leak_t, hgain, cow, how,
    out,
    rows, wg, psend, prev, wo, rim, inside, reach, states, sdecay, sin, sout,
    lcol, lrow, mix, osend, orecv,
    zs, zsl, zr, zloc, rs, rr, ts, tr, ps, pr, os_, or_, oloc, ms, mr, ss, sr, es, er,
):
    s, f, t = lax.axis_index("sp"), lax.axis_index("fs"), lax.axis_index("tp")
    other = 1 - t
    half = tok.shape[1]
    length = 2 * half
    kd = w0.shape[0]
    wide = w0.shape[1] // nf
    ws = (w3, w2, w4, w1, w0)
    np_ = len(ws)
    has_left, has_right = s > 0, s < ns - 1

    barrier = pltpu.get_barrier_semaphore()
    pl.semaphore_signal(barrier, inc=1, device_id={"tp": other}, device_id_type=MESH)
    for d in range(1, nf):
        pl.semaphore_signal(barrier, inc=1, device_id={"fs": f ^ d}, device_id_type=MESH)

    @pl.when(has_left)
    def _():
        pl.semaphore_signal(barrier, inc=1, device_id={"sp": s - 1}, device_id_type=MESH)

    @pl.when(has_right)
    def _():
        pl.semaphore_signal(barrier, inc=1, device_id={"sp": s + 1}, device_id_type=MESH)

    ends = jnp.where(has_left, 1, 0) + jnp.where(has_right, 1, 0)
    pl.semaphore_wait(barrier, nf + ends)

    def remote(src, dst, send, recv, **where):
        return pltpu.make_async_remote_copy(
            src_ref=src, dst_ref=dst, send_sem=send, recv_sem=recv,
            device_id=where, device_id_type=MESH,
        )

    def wblock(b, p):
        return wg.at[p, pl.ds(pl.multiple_of(b * kd, kd), kd), :]

    def wown(p):
        return ws[p].at[:, pl.ds(pl.multiple_of(f * wide, wide), wide)]

    def own_right(p):
        return remote(wown(p), wblock(s, p), zs.at[s, p], zr.at[s, p], sp=s + 1)

    def own_left(p):
        return remote(wown(p), wblock(s, p), zsl.at[p], zr.at[s, p], sp=s - 1)

    def relay(b, p, to):
        return remote(wblock(b, p), wblock(b, p), zs.at[b, p], zr.at[b, p], sp=to)

    def send_own(p):
        @pl.when(has_right)
        def _():
            own_right(p).start()

        @pl.when(has_left)
        def _():
            own_left(p).start()

        pltpu.make_async_copy(wown(p), wblock(s, p), zloc.at[p]).start()

    def zrelay(p):
        def hop(k, carry):
            @pl.when(s - k >= 0)
            def _():
                relay(s - k, p, s + 1).wait_recv()

                @pl.when(has_right)
                def _():
                    relay(s - k, p, s + 1).start()

            @pl.when(s + k < ns)
            def _():
                relay(s + k, p, s - 1).wait_recv()

                @pl.when(has_left)
                def _():
                    relay(s + k, p, s - 1).start()

            return carry

        lax.fori_loop(1, ns, hop, 0)
        pltpu.make_async_copy(wown(p), wblock(s, p), zloc.at[p]).wait()
        if p + 2 < np_:
            send_own(p + 2)

    send_own(0)
    send_own(1)

    x = tok[0].astype(F32)
    center = x - jnp.mean(x, axis=-1, keepdims=True)
    spread = jnp.mean(center * center, axis=-1, keepdims=True)
    rows[f, t] = (center * lax.rsqrt(spread + 1e-05) * gain[...]).astype(BF)

    quarter = half // 2

    def piece(g, j):
        return rows.at[g, t, pl.ds(j * quarter, quarter), :]

    def row_copy(g, j, to, slot):
        return remote(piece(g, j), piece(g, j), rs.at[slot], rr.at[g ^ f ^ to, j], fs=to)

    def row_arrived(d, j):
        g = f ^ d
        remote(piece(g, j), piece(g, j), rs.at[0], rr.at[d, j], fs=f ^ 1).wait_recv()

    def row_send(d, j, to_d, slot):
        g = f ^ d
        to = f ^ to_d
        return remote(piece(g, j), piece(g, j), rs.at[slot], rr.at[d ^ to_d, j], fs=to)

    def twin(d):
        g = f ^ d
        return remote(rows.at[g, t], rows.at[g, t], ts.at[d], tr.at[d], tp=other)

    def twin_arrived(d):
        g = f ^ d
        remote(rows.at[g, other], rows.at[g, other], ts.at[d], tr.at[d], tp=other).wait_recv()

    row_send(0, 0, 1, 0).start()
    row_send(0, 1, 2, 1).start()
    row_send(0, 1, 1, 2).start()
    row_send(0, 0, 2, 3).start()
    twin(0).start()

    ri = lax.broadcasted_iota(jnp.int32, (length, length), 0)
    ci = lax.broadcasted_iota(jnp.int32, (length, length), 1)
    tril = (ri >= ci).astype(F32)
    triu = (ri <= ci).astype(F32)
    high = lax.Precision.HIGHEST
    heads = leak.shape[2]
    lsum = jnp.dot(tril, leak[0], precision=high, preferred_element_type=F32)
    lsum_t = jnp.dot(leak_t[...], triu, precision=high, preferred_element_type=F32)
    for h in range(heads):
        lcol[h] = jnp.broadcast_to(lsum[:, h : h + 1], (length, wide))
        lrow[h] = jnp.broadcast_to(lsum_t[h : h + 1, :], (8, length))

    zrelay(0)
    row_arrived(1, 0)
    row_send(1, 0, 2, 4).start()
    row_arrived(2, 1)
    row_send(2, 1, 1, 5).start()
    zrelay(1)
    row_arrived(1, 1)
    twin(1).start()
    row_arrived(2, 0)
    twin(2).start()
    zrelay(2)
    row_arrived(3, 0)
    row_arrived(3, 1)
    twin(3).start()
    for d in range(nf):
        twin_arrived(d)

    def project(p):
        def one(g, carry):
            lhs = jnp.concatenate([rows[g, 0], rows[g, 1]], axis=0)
            psend[g, p] = jnp.dot(lhs, wg[p], preferred_element_type=F32).astype(BF)
            return carry

        lax.fori_loop(0, nf, one, 0)
        for d in range(1, nf):
            returned(d, p).start()
        prev[f, p] = psend[f, p]

    def returned(d, p):
        g = f ^ d
        return remote(psend.at[g, p], prev.at[f, p], ps.at[d, p], pr.at[d, p], fs=g)

    def returned_arrived(d, p):
        g = f ^ d
        remote(psend.at[g, p], prev.at[g, p], ps.at[d, p], pr.at[d, p], fs=g).wait_recv()

    project(0)
    project(1)
    project(2)
    zrelay(3)
    project(3)
    zrelay(4)
    project(4)

    outs = (cow, how)

    def own_out(j, to_d, slot):
        return remote(outs[j], wo.at[f, j], os_.at[slot], or_.at[to_d, j], fs=f ^ to_d)

    def relay_out(d, j, to_d, slot):
        g = f ^ d
        return remote(wo.at[g, j], wo.at[g, j], os_.at[slot], or_.at[d ^ to_d, j], fs=f ^ to_d)

    def out_arrived(d, j):
        g = f ^ d
        remote(wo.at[g, j], wo.at[g, j], os_.at[0], or_.at[d, j], fs=f ^ 1).wait_recv()

    own_out(0, 1, 0).start()
    own_out(1, 2, 1).start()
    own_out(1, 1, 2).start()
    own_out(0, 2, 3).start()
    for j in range(2):
        pltpu.make_async_copy(outs[j], wo.at[f, j], oloc.at[j]).start()

    for p in range(3):
        for d in range(1, nf):
            returned_arrived(d, p)
    causal = ri >= ci

    def local(h, carry):
        fl = floor[h]
        logits = prev[h, FORGET].astype(F32)
        retain = fl + (1.0 - fl) * jax.nn.sigmoid(logits)
        keys = (1.0 - fl) * jax.nn.sigmoid(-logits)
        total = jnp.dot(tril, jnp.log(retain), precision=high, preferred_element_type=F32)
        raw = prev[h, QUERY].astype(F32)
        query = raw * jax.nn.sigmoid(raw) * jnp.exp(total)
        value = prev[h, VALUE]
        scores = lax.dot_general(
            query.astype(BF), (keys * jnp.exp(-total)).astype(BF), NT, preferred_element_type=F32
        )
        lc = lcol[h]
        gap = lc[:, 0:1] - lrow[h, 0:1, :]
        scores = jnp.where(causal, scores * jnp.exp(jnp.where(causal, gap, 0.0)), 0.0)
        inside[h] = jnp.dot(scores.astype(BF), value, preferred_element_type=F32)
        reach[h] = (query * jnp.exp(lc)).astype(BF)
        full = total + lc
        end = full[length - 1 :, :]
        update = (keys * jnp.exp(end - full)).astype(BF)
        states[h] = lax.dot_general(value, update, TN, preferred_element_type=F32)
        sdecay[h] = jnp.broadcast_to(jnp.exp(end), (8, wide))
        return carry

    lax.fori_loop(0, heads, local, 0)

    for d in range(1, nf):
        returned_arrived(d, 3)
        returned_arrived(d, 4)
    edge = rim.shape[1]

    def rim_copy(g):
        return remote(
            prev.at[g, SIGNAL, pl.ds(length - edge, edge), :], rim.at[g],
            ms.at[g], mr.at[g], sp=s + 1,
        )

    for g in range(nf):
        @pl.when(has_right)
        def _(g=g):
            rim_copy(g).start()

        @pl.when(s == 0)
        def _(g=g):
            rim[g] = jnp.zeros((edge, wide), BF)

    def state_copy(h):
        return remote(sout.at[h], sin.at[h], ss.at[h], sr.at[h], sp=s + 1)

    def chain(h, carry):
        @pl.when(has_left)
        def _():
            state_copy(h).wait_recv()

        @pl.when(s == 0)
        def _():
            sin[h] = jnp.zeros(sin.shape[1:], BF)

        @pl.when(has_right)
        def _():
            sout[h] = (sin[h].astype(F32) * sdecay[h, 0:1, :] + states[h]).astype(BF)
            state_copy(h).start()

        raw = inside[h] + lax.dot_general(reach[h], sin[h], NT, preferred_element_type=F32)
        scale = lax.rsqrt(jnp.mean(raw * raw, axis=-1, keepdims=True) + 1e-06)
        mix[1, :, pl.ds(pl.multiple_of(h * wide, wide), wide)] = (
            raw * scale * hgain[...]
        ).astype(BF)
        return carry

    out_arrived(1, 0)
    relay_out(1, 0, 2, 4).start()
    out_arrived(2, 1)
    relay_out(2, 1, 1, 5).start()
    lax.fori_loop(0, heads, chain, 0)

    for g in range(nf):
        @pl.when(has_left)
        def _(g=g):
            rim_copy(g).wait_recv()

    def conv(g, carry):
        padded = jnp.concatenate([rim[g], prev[g, SIGNAL]], axis=0).astype(F32)
        margin = taps.shape[1] - 1
        filtered = jnp.zeros((length, wide), F32)
        for o in range(margin + 1):
            start = edge - margin + o
            filtered = filtered + taps[g, o : o + 1, :] * padded[start : start + length]
        mix[0, :, pl.ds(pl.multiple_of(g * wide, wide), wide)] = (
            prev[g, GATE].astype(F32) * filtered
        ).astype(BF)
        return carry

    lax.fori_loop(0, nf, conv, 0)

    def partial(c, who):
        at = pl.ds(pl.multiple_of(who * half, half), half)
        return jnp.dot(mix[0, at, :], wo[c, 0], preferred_element_type=F32) + jnp.dot(
            mix[1, at, :], wo[c, 1], preferred_element_type=F32
        )

    def share(d):
        return remote(osend.at[d], orecv.at[d], es.at[d], er.at[d], tp=other)

    for j in range(2):
        pltpu.make_async_copy(outs[j], wo.at[f, j], oloc.at[j]).wait()
    cols = wo.shape[3]
    for d in range(nf):
        if d:
            for j in range(2):
                if (d, j) not in ((1, 0), (2, 1)):
                    out_arrived(d, j)
        c = f ^ d
        osend[d] = partial(c, other)
        share(d).start()
        at = pl.ds(pl.multiple_of(c * cols, cols), cols)
        mine = partial(c, t)
        share(d).wait_recv()
        out[0, :, at] = (mine + orecv[d]).astype(BF)

    for p in range(np_):
        def drained(b, carry, p=p):
            @pl.when(((b < s) & has_right) | ((b > s) & has_left))
            def _():
                relay(b, p, s).wait_send()

            return carry

        lax.fori_loop(0, ns, drained, 0)

        @pl.when(has_right)
        def _(p=p):
            own_right(p).wait_send()

        @pl.when(has_left)
        def _(p=p):
            own_left(p).wait_send()

        for d in range(1, nf):
            returned(d, p).wait_send()
    for d, j, to_d, slot in ((0, 0, 1, 0), (0, 1, 2, 1), (0, 1, 1, 2), (0, 0, 2, 3), (1, 0, 2, 4), (2, 1, 1, 5)):
        row_send(d, j, to_d, slot).wait_send()
        if d == 0:
            own_out(j, to_d, slot).wait_send()
        else:
            relay_out(d, j, to_d, slot).wait_send()
    for d in range(nf):
        twin(d).wait_send()
        share(d).wait_send()

    @pl.when(has_right)
    def _():
        for h in range(heads):
            state_copy(h).wait_send()
        for g in range(nf):
            rim_copy(g).wait_send()


def body(ns, nf, tokens, norm_gain, w0, w1, w2, w3, w4, conv_taps, floor_gate, leak, head_gain, cow, how):
    half, width = tokens.shape[1:]
    length = 2 * half
    heads = leak.shape[2]
    kd = w0.shape[0]
    wide = w0.shape[1] // nf
    assert heads == nf and nf == 4 and floor_gate.shape[0] == heads * wide
    taps = conv_taps.reshape(conv_taps.shape[0], nf, wide).transpose(1, 0, 2)
    vm = pl.BlockSpec(memory_space=pltpu.VMEM)
    dma = pltpu.SemaphoreType.DMA
    scratch = [
        pltpu.VMEM((nf, 2, half, width), BF),
        pltpu.VMEM((5, ns * kd, wide), BF),
        pltpu.VMEM((nf, 5, length, wide), BF),
        pltpu.VMEM((nf, 5, length, wide), BF),
        pltpu.VMEM((nf, 2) + cow.shape, BF),
        pltpu.VMEM((nf, 16, wide), BF),
        pltpu.VMEM((heads, length, wide), F32),
        pltpu.VMEM((heads, length, wide), BF),
        pltpu.VMEM((heads, wide, wide), F32),
        pltpu.VMEM((heads, 8, wide), F32),
        pltpu.VMEM((heads, wide, wide), BF),
        pltpu.VMEM((heads, wide, wide), BF),
        pltpu.VMEM((heads, length, wide), F32),
        pltpu.VMEM((heads, 8, length), F32),
        pltpu.VMEM((2, length, heads * wide), BF),
        pltpu.VMEM((nf, half, cow.shape[1]), F32),
        pltpu.VMEM((nf, half, cow.shape[1]), F32),
        dma((ns, 5)), dma((5,)), dma((ns, 5)), dma((5,)),
        dma((6,)), dma((nf, 2)), dma((nf,)), dma((nf,)),
        dma((nf, 5)), dma((nf, 5)),
        dma((6,)), dma((nf, 2)), dma((2,)),
        dma((nf,)), dma((nf,)), dma((heads,)), dma((heads,)),
        dma((nf,)), dma((nf,)),
    ]
    return pl.pallas_call(
        functools.partial(kernel, ns, nf),
        out_shape=jax.ShapeDtypeStruct(tokens.shape, BF),
        in_specs=[vm] * 14,
        out_specs=vm,
        scratch_shapes=scratch,
        compiler_params=pltpu.CompilerParams(
            collective_id=0, has_side_effects=True, vmem_limit_bytes=60 * 2**20
        ),
    )(
        tokens, norm_gain[None], w0, w1, w2, w3, w4, taps, floor_gate.reshape(heads, 1, wide),
        leak, leak[0].T, head_gain[None], cow, how,
    )


def solution(mesh):
    in_specs = (
        P("fs", ("sp", "tp"), None),
        P(),
        P("sp", "tp"),
        P("sp", "tp"),
        P("sp", "tp"),
        P("sp", "tp"),
        P("sp", "tp"),
        P(None, "tp"),
        P("tp"),
        P("fs", "sp", "tp"),
        P(),
        P("tp", "fs"),
        P("tp", "fs"),
    )
    out_specs = P("fs", ("sp", "tp"), None)
    step = functools.partial(body, mesh.shape["sp"], mesh.shape["fs"])
    return jax.shard_map(step, mesh=mesh, in_specs=in_specs, out_specs=out_specs, check_vma=False)
```

```python
import functools

import jax
import jax.numpy as jnp
from jax import lax
from jax.experimental import pallas as pl
from jax.experimental.pallas import tpu as pltpu
from jax.sharding import PartitionSpec as P

MESH = pl.DeviceIdType.MESH
BF = jnp.bfloat16
F32 = jnp.float32
NT = (((1,), (1,)), ((), ()))
TN = (((0,), (0,)), ((), ()))
GATE, SIGNAL, QUERY, FORGET, VALUE = 4, 3, 1, 0, 2


def kernel(
    ns, nf,
    tok, gain, w0, w1, w2, w3, w4, taps, floor, leak, leak_t, hgain, cow, how,
    out,
    rows, wg, psend, prev, wo, rim, inside, reach, states, sdecay, sin, sout,
    lcol, lrow, mix, osend, orecv, through,
    zs, zsl, zr, zloc, rs, rr, ts, tr, ps, pr, os_, or_, oloc, ms, mr, ss, sr, es, er, ds, dr, ns_, nr,
):
    s, f, t = lax.axis_index("sp"), lax.axis_index("fs"), lax.axis_index("tp")
    other = 1 - t
    half = tok.shape[1]
    length = 2 * half
    kd = w0.shape[0]
    wide = w0.shape[1] // nf
    ws = (w3, w2, w4, w1, w0)
    np_ = len(ws)
    has_left, has_right = s > 0, s < ns - 1

    barrier = pltpu.get_barrier_semaphore()
    pl.semaphore_signal(barrier, inc=1, device_id={"tp": other}, device_id_type=MESH)
    for d in range(1, nf):
        pl.semaphore_signal(barrier, inc=1, device_id={"fs": f ^ d}, device_id_type=MESH)

    @pl.when(has_left)
    def _():
        pl.semaphore_signal(barrier, inc=1, device_id={"sp": s - 1}, device_id_type=MESH)

    @pl.when(has_right)
    def _():
        pl.semaphore_signal(barrier, inc=1, device_id={"sp": s + 1}, device_id_type=MESH)

    ends = jnp.where(has_left, 1, 0) + jnp.where(has_right, 1, 0)
    pl.semaphore_wait(barrier, nf + ends)

    def remote(src, dst, send, recv, **where):
        return pltpu.make_async_remote_copy(
            src_ref=src, dst_ref=dst, send_sem=send, recv_sem=recv,
            device_id=where, device_id_type=MESH,
        )

    def wblock(b, p):
        return wg.at[p, pl.ds(pl.multiple_of(b * kd, kd), kd), :]

    def wown(p):
        return ws[p].at[:, pl.ds(pl.multiple_of(f * wide, wide), wide)]

    def own_right(p):
        return remote(wown(p), wblock(s, p), zs.at[s, p], zr.at[s, p], sp=s + 1)

    def own_left(p):
        return remote(wown(p), wblock(s, p), zsl.at[p], zr.at[s, p], sp=s - 1)

    def relay(b, p, to):
        return remote(wblock(b, p), wblock(b, p), zs.at[b, p], zr.at[b, p], sp=to)

    def send_own(p):
        @pl.when(has_right)
        def _():
            own_right(p).start()

        @pl.when(has_left)
        def _():
            own_left(p).start()

        pltpu.make_async_copy(wown(p), wblock(s, p), zloc.at[p]).start()

    def zrelay(p):
        def hop(k, carry):
            @pl.when(s - k >= 0)
            def _():
                relay(s - k, p, s + 1).wait_recv()

                @pl.when(has_right)
                def _():
                    relay(s - k, p, s + 1).start()

            @pl.when(s + k < ns)
            def _():
                relay(s + k, p, s - 1).wait_recv()

                @pl.when(has_left)
                def _():
                    relay(s + k, p, s - 1).start()

            return carry

        lax.fori_loop(1, ns, hop, 0)
        pltpu.make_async_copy(wown(p), wblock(s, p), zloc.at[p]).wait()
        if p + 2 < np_:
            send_own(p + 2)

    send_own(0)
    send_own(1)

    x = tok[0].astype(F32)
    center = x - jnp.mean(x, axis=-1, keepdims=True)
    spread = jnp.mean(center * center, axis=-1, keepdims=True)
    rows[f, pl.ds(pl.multiple_of(t * half, half), half), :] = (
        center * lax.rsqrt(spread + 1e-05) * gain[...]
    ).astype(BF)

    quarter = half // 2

    def piece(g, j):
        return rows.at[g, pl.ds(pl.multiple_of(t * half + j * quarter, quarter), quarter), :]

    def core_rows(g, core):
        return rows.at[g, pl.ds(pl.multiple_of(core * half, half), half), :]

    def row_arrived(d, j):
        g = f ^ d
        remote(piece(g, j), piece(g, j), rs.at[0], rr.at[d, j], fs=f ^ 1).wait_recv()

    def row_send(d, j, to_d, slot):
        g = f ^ d
        to = f ^ to_d
        return remote(piece(g, j), piece(g, j), rs.at[slot], rr.at[d ^ to_d, j], fs=to)

    def twin(d):
        g = f ^ d
        return remote(core_rows(g, t), core_rows(g, t), ts.at[d], tr.at[d], tp=other)

    def twin_arrived(d):
        g = f ^ d
        remote(core_rows(g, other), core_rows(g, other), ts.at[d], tr.at[d], tp=other).wait_recv()

    row_send(0, 0, 1, 0).start()
    row_send(0, 1, 2, 1).start()
    row_send(0, 1, 1, 2).start()
    row_send(0, 0, 2, 3).start()
    twin(0).start()

    ri = lax.broadcasted_iota(jnp.int32, (length, length), 0)
    ci = lax.broadcasted_iota(jnp.int32, (length, length), 1)
    tril = (ri >= ci).astype(F32)
    triu = (ri <= ci).astype(F32)
    high = lax.Precision.HIGHEST
    heads = leak.shape[2]
    lsum = jnp.dot(tril, leak[0], precision=high, preferred_element_type=F32)
    lsum_t = jnp.dot(leak_t[...], triu, precision=high, preferred_element_type=F32)
    for h in range(heads):
        lcol[h] = jnp.broadcast_to(lsum[:, h : h + 1], (length, wide))
        lrow[h] = jnp.broadcast_to(lsum_t[h : h + 1, :], (8, length))

    outs = (cow, how)

    def own_out(j, to_d, slot):
        return remote(outs[j], wo.at[f, j], os_.at[slot], or_.at[to_d, j], fs=f ^ to_d)

    def relay_out(d, j, to_d, slot):
        g = f ^ d
        return remote(wo.at[g, j], wo.at[g, j], os_.at[slot], or_.at[d ^ to_d, j], fs=f ^ to_d)

    def out_arrived(d, j):
        g = f ^ d
        remote(wo.at[g, j], wo.at[g, j], os_.at[0], or_.at[d, j], fs=f ^ 1).wait_recv()

    for j in range(2):
        pltpu.make_async_copy(outs[j], wo.at[f, j], oloc.at[j]).start()

    zrelay(0)
    row_arrived(1, 0)
    row_send(1, 0, 2, 4).start()
    row_arrived(2, 1)
    row_send(2, 1, 1, 5).start()
    own_out(0, 1, 0).start()
    own_out(1, 2, 1).start()
    zrelay(1)
    row_arrived(1, 1)
    twin(1).start()
    row_arrived(2, 0)
    twin(2).start()
    zrelay(2)
    row_arrived(3, 0)
    row_arrived(3, 1)
    twin(3).start()
    for d in range(nf):
        twin_arrived(d)

    def project(p):
        def one(g, carry):
            psend[g, p] = jnp.dot(rows[g], wg[p], preferred_element_type=F32).astype(BF)
            return carry

        lax.fori_loop(0, nf, one, 0)
        for d in range(1, nf):
            returned(d, p).start()
        prev[f, p] = psend[f, p]

    def returned(d, p):
        g = f ^ d
        return remote(psend.at[g, p], prev.at[f, p], ps.at[d, p], pr.at[d, p], fs=g)

    def returned_arrived(d, p):
        g = f ^ d
        remote(psend.at[g, p], prev.at[g, p], ps.at[d, p], pr.at[d, p], fs=g).wait_recv()

    def gathered(p):
        for d in range(1, nf):
            returned_arrived(d, p)

    project(0)
    project(1)
    project(2)
    own_out(1, 1, 2).start()
    own_out(0, 2, 3).start()
    zrelay(3)
    project(3)
    zrelay(4)
    project(4)
    out_arrived(1, 0)
    relay_out(1, 0, 2, 4).start()
    out_arrived(2, 1)
    relay_out(2, 1, 1, 5).start()

    for p in range(3):
        gathered(p)
    causal = ri >= ci
    tril_short = tril.astype(BF)

    def local(h, carry):
        fl = floor[h]
        logits = prev[h, FORGET].astype(F32)
        retain = fl + (1.0 - fl) * jax.nn.sigmoid(logits)
        keys = (1.0 - fl) * jax.nn.sigmoid(-logits)
        step = jnp.log(retain)
        coarse = step.astype(BF)
        fine = (step - coarse.astype(F32)).astype(BF)
        both = jnp.dot(
            tril_short, jnp.concatenate([coarse, fine], axis=1), preferred_element_type=F32
        )
        total = both[:, :wide] + both[:, wide:]
        raw = prev[h, QUERY].astype(F32)
        query = raw * jax.nn.sigmoid(raw) * jnp.exp(total)
        value = prev[h, VALUE]
        scores = lax.dot_general(
            query.astype(BF), (keys * jnp.exp(-total)).astype(BF), NT, preferred_element_type=F32
        )
        lc = lcol[h]
        gap = lc[:, 0:1] - lrow[h, 0:1, :]
        scores = jnp.where(causal, scores * jnp.exp(jnp.where(causal, gap, 0.0)), 0.0)
        inside[h] = jnp.dot(scores.astype(BF), value, preferred_element_type=F32)
        reach[h] = (query * jnp.exp(lc)).astype(BF)
        full = total + lc
        end = full[length - 1 :, :]
        update = (keys * jnp.exp(end - full)).astype(BF)
        states[h] = lax.dot_general(value, update, TN, preferred_element_type=F32)
        sdecay[h] = jnp.broadcast_to(jnp.exp(end), (8, wide))
        return carry

    lax.fori_loop(0, heads, local, 0)

    gathered(3)
    edge = rim.shape[1]

    def rim_copy(g):
        return remote(
            prev.at[g, SIGNAL, pl.ds(length - edge, edge), :], rim.at[g],
            ms.at[g], mr.at[g], sp=s + 1,
        )

    for g in range(nf):
        @pl.when(has_right)
        def _(g=g):
            rim_copy(g).start()

        @pl.when(s == 0)
        def _(g=g):
            rim[g] = jnp.zeros((edge, wide), BF)

    def state_copy(h):
        return remote(sout.at[h], sin.at[h], ss.at[h], sr.at[h], sp=s + 1)

    def chain(h, carry):
        @pl.when(has_left)
        def _():
            state_copy(h).wait_recv()

        @pl.when(s == 0)
        def _():
            sin[h] = jnp.zeros(sin.shape[1:], BF)

        @pl.when(has_right)
        def _():
            sout[h] = (sin[h].astype(F32) * sdecay[h, 0:1, :] + states[h]).astype(BF)
            state_copy(h).start()

        raw = inside[h] + lax.dot_general(reach[h], sin[h], NT, preferred_element_type=F32)
        scale = lax.rsqrt(jnp.mean(raw * raw, axis=-1, keepdims=True) + 1e-06)
        mix[1, :, pl.ds(pl.multiple_of(h * wide, wide), wide)] = (
            raw * scale * hgain[...]
        ).astype(BF)
        return carry

    lax.fori_loop(0, heads, chain, 0)
    gathered(4)

    for g in range(nf):
        @pl.when(has_left)
        def _(g=g):
            rim_copy(g).wait_recv()

    def conv(g, carry):
        padded = jnp.concatenate([rim[g], prev[g, SIGNAL]], axis=0).astype(F32)
        margin = taps.shape[1] - 1
        filtered = jnp.zeros((length, wide), F32)
        for o in range(margin + 1):
            start = edge - margin + o
            filtered = filtered + taps[g, o : o + 1, :] * padded[start : start + length]
        mix[0, :, pl.ds(pl.multiple_of(g * wide, wide), wide)] = (
            prev[g, GATE].astype(F32) * filtered
        ).astype(BF)
        return carry

    lax.fori_loop(0, nf, conv, 0)

    def partial(c, who):
        at = pl.ds(pl.multiple_of(who * half, half), half)
        return jnp.dot(mix[0, at, :], wo[c, 0], preferred_element_type=F32) + jnp.dot(
            mix[1, at, :], wo[c, 1], preferred_element_type=F32
        )

    def share(d):
        return remote(osend.at[d], orecv.at[d], es.at[d], er.at[d], tp=other)

    for j in range(2):
        pltpu.make_async_copy(outs[j], wo.at[f, j], oloc.at[j]).wait()
    cols = wo.shape[3]
    for d in range(nf):
        if d:
            for j in range(2):
                if (d, j) not in ((1, 0), (2, 1)):
                    out_arrived(d, j)
        c = f ^ d
        osend[d] = partial(c, other)
        share(d).start()
        at = pl.ds(pl.multiple_of(c * cols, cols), cols)
        mine = partial(c, t)
        share(d).wait_recv()
        out[0, :, at] = (mine + orecv[d]).astype(BF)

    for p in range(np_):
        def drained(b, carry, p=p):
            @pl.when(((b < s) & has_right) | ((b > s) & has_left))
            def _():
                relay(b, p, s).wait_send()

            return carry

        lax.fori_loop(0, ns, drained, 0)

        @pl.when(has_right)
        def _(p=p):
            own_right(p).wait_send()

        @pl.when(has_left)
        def _(p=p):
            own_left(p).wait_send()

        for d in range(1, nf):
            returned(d, p).wait_send()
    for d, j, to_d, slot in ((0, 0, 1, 0), (0, 1, 2, 1), (0, 1, 1, 2), (0, 0, 2, 3), (1, 0, 2, 4), (2, 1, 1, 5)):
        row_send(d, j, to_d, slot).wait_send()
        if d == 0:
            own_out(j, to_d, slot).wait_send()
        else:
            relay_out(d, j, to_d, slot).wait_send()
    for d in range(nf):
        twin(d).wait_send()
        share(d).wait_send()

    @pl.when(has_right)
    def _():
        for h in range(heads):
            state_copy(h).wait_send()
        for g in range(nf):
            rim_copy(g).wait_send()


def body(ns, nf, tokens, norm_gain, w0, w1, w2, w3, w4, conv_taps, floor_gate, leak, head_gain, cow, how):
    half, width = tokens.shape[1:]
    length = 2 * half
    heads = leak.shape[2]
    kd = w0.shape[0]
    wide = w0.shape[1] // nf
    assert heads == nf and nf == 4 and floor_gate.shape[0] == heads * wide
    taps = conv_taps.reshape(conv_taps.shape[0], nf, wide).transpose(1, 0, 2)
    vm = pl.BlockSpec(memory_space=pltpu.VMEM)
    dma = pltpu.SemaphoreType.DMA
    scratch = [
        pltpu.VMEM((nf, length, width), BF),
        pltpu.VMEM((5, ns * kd, wide), BF),
        pltpu.VMEM((nf, 5, length, wide), BF),
        pltpu.VMEM((nf, 5, length, wide), BF),
        pltpu.VMEM((nf, 2) + cow.shape, BF),
        pltpu.VMEM((nf, 16, wide), BF),
        pltpu.VMEM((heads, length, wide), F32),
        pltpu.VMEM((heads, length, wide), BF),
        pltpu.VMEM((heads, wide, wide), F32),
        pltpu.VMEM((heads, 8, wide), F32),
        pltpu.VMEM((heads, wide, wide), BF),
        pltpu.VMEM((heads, wide, wide), BF),
        pltpu.VMEM((heads, length, wide), F32),
        pltpu.VMEM((heads, 8, length), F32),
        pltpu.VMEM((2, length, heads * wide), BF),
        pltpu.VMEM((nf, half, cow.shape[1]), F32),
        pltpu.VMEM((nf, half, cow.shape[1]), F32),
        pltpu.VMEM((2, 5, half, wide), BF),
        dma((ns, 5)), dma((5,)), dma((ns, 5)), dma((5,)),
        dma((6,)), dma((nf, 2)), dma((nf,)), dma((nf,)),
        dma((nf, 5)), dma((nf, 5)),
        dma((6,)), dma((nf, 2)), dma((2,)),
        dma((nf,)), dma((nf,)), dma((heads,)), dma((heads,)),
        dma((nf,)), dma((nf,)),
        dma((2, 5)), dma((2, 5)), dma((2, 5)), dma((2, 5)),
    ]
    return pl.pallas_call(
        functools.partial(kernel, ns, nf),
        out_shape=jax.ShapeDtypeStruct(tokens.shape, BF),
        in_specs=[vm] * 14,
        out_specs=vm,
        scratch_shapes=scratch,
        compiler_params=pltpu.CompilerParams(
            collective_id=0, has_side_effects=True, vmem_limit_bytes=60 * 2**20
        ),
    )(
        tokens, norm_gain[None], w0, w1, w2, w3, w4, taps, floor_gate.reshape(heads, 1, wide),
        leak, leak[0].T, head_gain[None], cow, how,
    )


def solution(mesh):
    in_specs = (
        P("fs", ("sp", "tp"), None),
        P(),
        P("sp", "tp"),
        P("sp", "tp"),
        P("sp", "tp"),
        P("sp", "tp"),
        P("sp", "tp"),
        P(None, "tp"),
        P("tp"),
        P("fs", "sp", "tp"),
        P(),
        P("tp", "fs"),
        P("tp", "fs"),
    )
    out_specs = P("fs", ("sp", "tp"), None)
    step = functools.partial(body, mesh.shape["sp"], mesh.shape["fs"])
    return jax.shard_map(step, mesh=mesh, in_specs=in_specs, out_specs=out_specs, check_vma=False)
```
